128 devices in a mesh: fs: 16 (over z, y), rep: 4 (over x), tp: 2 (over core).
Axes of the slice: x: 4, y: 4, z: 4, core: 2. Of those that a mesh axis runs over, the one named last changes fastest.
Arguments:
- normed_in: bfloat16 [98304, 2048], P(('fs', 'rep')), may hold values from -6 to 6
- cotan_rec: bfloat16 [98304, 2048], P(('fs', 'rep'), 'tp'), may hold values from -0.01953125 to 0.01953125
- cotan_gate: bfloat16 [98304, 2048], P(('fs', 'rep'), 'tp'), may hold values from -0.01953125 to 0.01953125
- factor_rec: bfloat16 [2048, 512], P('fs'), may hold values from -0.125 to 0.125
- factor_gate: bfloat16 [2048, 512], P('fs'), may hold values from -0.125 to 0.125
- first_rec: float32 [512, 2048], P('fs', 'tp'), may hold values from -6 to 6
- first_gate: float32 [512, 2048], P('fs', 'tp'), may hold values from -6 to 6
- second_rec: float32 [512, 2048], P('fs', 'tp'), may hold values from 0.25 to 4
- second_gate: float32 [512, 2048], P('fs', 'tp'), may hold values from 0.25 to 4
- master_rec: float32 [2048, 2048], P('fs', 'tp'), may hold values from -0.125 to 0.125
- master_gate: float32 [2048, 2048], P('fs', 'tp'), may hold values from -0.125 to 0.125
Outputs:
- update_rec: float32 [2048, 2048], P('fs', 'tp')
- update_gate: float32 [2048, 2048], P('fs', 'tp')
- new_first_rec: float32 [512, 2048], P('fs', 'tp')
- new_first_gate: float32 [512, 2048], P('fs', 'tp')
- new_second_rec: float32 [512, 2048], P('fs', 'tp')
- new_second_gate: float32 [512, 2048], P('fs', 'tp')
- copy_rec: bfloat16 [2048, 2048], P(None, 'tp')
- copy_gate: bfloat16 [2048, 2048], P(None, 'tp')
The draws below stay inside these ranges and needn't reach their ends.
All inputs are finite; a program needn't handle non-finite values.
Results may differ from the reference program's by a relative error of at most 0.007.
Values may be sent and summed in bfloat16 or wider, within the bound.
A program may use at most 128 MiB of HBM per device.

```python
import math
import jax
import jax.numpy as jnp
from jax import lax

D = 2048
DR = 2048
RANK = 512
TOKENS = 98304


def shard_levels(stream_key, shape, pieces, smallest, largest):
    loudness, own = 1.0, jax.random.fold_in(stream_key, 6)
    for axis_at, shards_of in pieces:
        heights = jnp.exp(jax.random.uniform(jax.random.fold_in(own, axis_at), (shards_of,), jnp.float32, smallest / len(pieces), largest / len(pieces)))
        loudness = loudness * jnp.repeat(heights, shape[axis_at] // shards_of).reshape([-1 if axis == axis_at else 1 for axis in range(len(shape))])
    return loudness


def centred(key, shape, scale, limit, cuts=(), dtype=jnp.bfloat16):
    factor_of = shard_levels(key, shape, cuts, -0.22, 0.18) if cuts else 1.0
    drawn = jax.random.normal(key, shape, jnp.float32) * scale * factor_of
    return jnp.minimum(jnp.maximum(drawn, -limit), limit).astype(dtype)


def setup_inputs(seed: int = 0) -> dict:
    key_of = jax.random.split(jax.random.key(seed), 12)
    return {
        "normed_in": centred(key_of[0], (TOKENS, D), 1.0, 6.0, ((0, 64),)),
        "cotan_rec": centred(key_of[1], (TOKENS, DR), (TOKENS ** -0.5), 0.01953125, ((0, 64), (1, 2))),
        "cotan_gate": centred(key_of[2], (TOKENS, DR), (TOKENS ** -0.5), 0.01953125, ((0, 64), (1, 2))),
        "factor_rec": centred(key_of[3], (D, RANK), D ** -0.5, 0.125, ((0, 16),)),
        "factor_gate": centred(key_of[4], (D, RANK), D ** -0.5, 0.125, ((0, 16),)),
        "first_rec": centred(key_of[5], (RANK, DR), 1.0, 6.0, ((0, 16), (1, 2)), jnp.float32),
        "first_gate": centred(key_of[6], (RANK, DR), 1.0, 6.0, ((0, 16), (1, 2)), jnp.float32),
        "second_rec": jnp.clip(jnp.exp(math.log(4.0) - 2.7725887 * jax.random.uniform(key_of[7], (RANK, DR), jnp.float32) ** shard_levels(key_of[7], (RANK, DR), ((0, 16), (1, 2)), -0.2, 0.2)), 0.25, 4.0),
        "second_gate": jnp.clip(jnp.exp(math.log(4.0) - 2.7725887 * jax.random.uniform(key_of[8], (RANK, DR), jnp.float32) ** shard_levels(key_of[8], (RANK, DR), ((0, 16), (1, 2)), -0.2, 0.2)), 0.25, 4.0),
        "master_rec": centred(key_of[9], (D, DR), D ** -0.5, 0.125, ((0, 16), (1, 2)), jnp.float32),
        "master_gate": centred(key_of[10], (D, DR), D ** -0.5, 0.125, ((0, 16), (1, 2)), jnp.float32),
    }


beta_first = 0.8
beta_second = 0.9
scale_floor = 0.25
step_rate = 0.01

def project_update(normed_in, cotan, factor, first, second, master):
    grad = lax.dot_general(normed_in, cotan, (((0,), (0,)), ((), ())), preferred_element_type=jnp.float32)
    factor_wide = factor.astype(jnp.float32)
    low = jnp.dot(factor_wide.T, grad, precision=lax.Precision.HIGHEST)
    new_first = beta_first * first + (1.0 - beta_first) * low
    new_second = beta_second * second + (1.0 - beta_second) * low * low
    direction = new_first / jnp.sqrt(new_second)
    scale = 1.0 / jnp.sqrt(jnp.mean(direction * direction) + scale_floor)
    update = jnp.dot(factor_wide, direction, precision=lax.Precision.HIGHEST) * scale
    copy = (master - step_rate * update).astype(jnp.bfloat16)
    return (update, new_first, new_second, copy)

def reference(normed_in, cotan_rec, cotan_gate, factor_rec, factor_gate, first_rec, first_gate, second_rec, second_gate, master_rec, master_gate):
    upd_rec, first_r, second_r, copy_rec = project_update(normed_in, cotan_rec, factor_rec, first_rec, second_rec, master_rec)
    upd_gate, first_g, second_g, copy_gate = project_update(normed_in, cotan_gate, factor_gate, first_gate, second_gate, master_gate)
    return (upd_rec, upd_gate, first_r, first_g, second_r, second_g, copy_rec, copy_gate)
```

```python
import jax
import jax.numpy as jnp
from jax import lax
from jax.experimental import pallas as pl
from jax.experimental.pallas import tpu as pltpu
from jax.sharding import PartitionSpec as P

MESH = pl.DeviceIdType.MESH
BF = jnp.bfloat16
F32 = jnp.float32

D = 2048
DR = 2048
RANK = 512
ENTRIES = float(RANK * DR)
TOK = 1536
HALF = 1024

beta_first = 0.8
beta_second = 0.9
scale_floor = 0.25
step_rate = 0.01

GATHER_ORDER = (("x", "y", "z"), ("y", "z", "x"), ("z", "x", "y"))
COLS = ((0, 384), (384, 384), (768, 256))
SPLIT = (256, 128, 128)
WIDE_COLS = ((0, 640), (640, 640), (1280, 768))
N_SEMS = 172


def ring_kernel(
    normed_ref,
    cot_rec_ref,
    cot_gate_ref,
    fac_rec_ref,
    fac_gate_ref,
    first_rec_ref,
    first_gate_ref,
    second_rec_ref,
    second_gate_ref,
    master_rec_ref,
    master_gate_ref,
    fac,
    direc,
    mast,
    lowx,
    sq,
    xs,
    cots,
    proj_t,
    part,
    moms,
    mast_f,
    low,
    sq_own,
    sq_other,
    lefts,
    left_ones,
    rights,
    right_ones,
    send_sems,
    recv_sems,
    local_sems,
):
    f, x, c = lax.axis_index("fs"), lax.axis_index("rep"), lax.axis_index("tp")
    me = {"x": x, "y": lax.rem(f, 4), "z": lax.div(f, 4)}
    count = [0]
    started = []

    def coord(dim, delta):
        return lax.rem(me[dim] + (delta + 4) % 4, 4)

    def device(dim, delta):
        if dim == "core":
            return {"tp": 1 - c}
        p = coord(dim, delta)
        if dim == "x":
            return {"rep": p}
        if dim == "y":
            return {"fs": me["z"] * 4 + p}
        return {"fs": p * 4 + me["y"]}

    def send(src, dst, dim, delta):
        k = count[0]
        count[0] += 1
        copy = pltpu.make_async_remote_copy(
            src_ref=src,
            dst_ref=dst,
            send_sem=send_sems.at[k],
            recv_sem=recv_sems.at[k],
            device_id=device(dim, delta),
            device_id_type=MESH,
        )
        copy.start()
        started.append(copy)
        return copy

    def full(v):
        return slice(None) if v is None else v

    def rank_index(at):
        xx = at["x"]
        if xx is None:
            return (slice(None), full(at["z"]), full(at["y"]), slice(None))
        return (lax.div(xx, 2), full(at["z"]), full(at["y"]), lax.rem(xx, 2))

    def fac_index(at):
        return (full(at["z"]), full(at["y"]), full(at["x"]), c)

    def mast_index(at):
        return (full(at["z"]), full(at["y"]), full(at["x"]))

    def col_parts(s):
        base, width = COLS[s]
        one = SPLIT[s]
        rows = slice(None)
        return (
            (rows, pl.ds(base, width)),
            (rows, pl.ds(base, one)),
            (rows, pl.ds(base + one, width - one)),
        )

    def row_parts(s):
        base, width = WIDE_COLS[s]
        cols = pl.ds(base, width)
        return ((slice(None), cols), (pl.ds(0, 16), cols), (pl.ds(16, 16), cols))

    def gather(buf, index, parts):
        for k in range(3):
            sent = []
            for s in range(3):
                order = GATHER_ORDER[s]
                at = {d: (None if d in order[:k] else me[d]) for d in order}
                whole, _, _ = parts(s)
                view = buf.at[index(at) + whole]
                sent.append(
                    (send(view, view, order[k], 1), send(view, view, order[k], -1))
                )
            yield
            passed = []
            for s in range(3):
                order = GATHER_ORDER[s]
                _, one, two = parts(s)
                at = {d: (None if d in order[:k] else me[d]) for d in order}
                sent[s][0].wait_recv()
                at[order[k]] = coord(order[k], -1)
                view = buf.at[index(at) + one]
                a = send(view, view, order[k], 1)
                sent[s][1].wait_recv()
                at[order[k]] = coord(order[k], 1)
                view = buf.at[index(at) + two]
                b = send(view, view, order[k], -1)
                passed.append((a, b))
            yield
            for a, b in passed:
                a.wait_recv()
                b.wait_recv()
        yield

    local = []

    def fetch(src, dst):
        copy = pltpu.make_async_copy(src, dst, local_sems.at[len(local)])
        copy.start()
        local.append(copy)
        return copy

    own_rows = pl.ds(pl.multiple_of((2 * x + c) * 16, 16), 16)
    own_fac = fac_index(me)
    fac_in = [
        fetch(r.at[own_rows], fac.at[own_fac + (slice(None), pl.ds(512 * m, 512))])
        for m, r in enumerate((fac_rec_ref, fac_gate_ref))
    ]
    quarter = pl.ds(pl.multiple_of(x * 32, 32), 32)
    mast_in = [
        fetch(r.at[quarter], mast_f.at[m])
        for m, r in enumerate((master_rec_ref, master_gate_ref))
    ]
    x_in = [
        fetch(normed_ref.at[pl.ds(256 * i, 256)], xs.at[i]) for i in range(6)
    ]
    cot_in = [fetch(r, cots.at[m]) for m, r in enumerate((cot_rec_ref, cot_gate_ref))]
    mom_in = [
        fetch(r, moms.at[i])
        for i, r in enumerate(
            (first_rec_ref, first_gate_ref, second_rec_ref, second_gate_ref)
        )
    ]

    barrier = pltpu.get_barrier_semaphore()
    for dim, delta in (("x", 1), ("x", -1), ("y", 1), ("y", -1), ("z", 1), ("z", -1), ("core", 0)):
        pl.semaphore_signal(
            barrier, inc=1, device_id=device(dim, delta), device_id_type=MESH
        )
    for copy in mast_in:
        copy.wait()
    own_mast = mast_index(me)
    for m in range(2):
        mast[own_mast + (slice(None), pl.ds(1024 * m, 1024))] = mast_f[m].astype(BF)
    for copy in fac_in:
        copy.wait()
    pl.semaphore_wait(barrier, 7)

    facs = gather(fac, fac_index, col_parts)
    masts = gather(mast, mast_index, row_parts)
    for _ in range(2):
        next(facs)
        next(masts)
    for _ in range(4):
        next(facs)
    next(masts)
    next(facs)
    swap = []
    for s in range(3):
        whole = col_parts(s)[0]
        view = fac.at[(slice(None), slice(None), slice(None), c) + whole]
        swap.append(send(view, view, "core", 0))
    next(masts)
    for copy in swap:
        copy.wait_recv()
    for copy in x_in:
        copy.wait()

    def project(lo, hi):
        def one(i, carry):
            tokens = pl.ds(pl.multiple_of(i * 256, 256), 256)
            for m in range(2):
                cols = pl.ds(512 * m, 512)
                factor = fac[:, :, :, :, :, cols].reshape(D, 512)
                got = jnp.dot(xs[i], factor, preferred_element_type=F32)
                proj_t[m, :, tokens] = got.astype(BF).T
            return carry

        lax.fori_loop(lo, hi, one, 0)

    project(0, 3)
    next(masts)
    project(3, 6)
    for copy in cot_in:
        copy.wait()

    for m in range(2):

        def one(j, carry):
            cols = pl.ds(pl.multiple_of(j * 512, 512), 512)
            got = jnp.dot(proj_t[m], cots[m, :, cols], preferred_element_type=F32)
            part[m, :, :, :, :, cols] = got.astype(BF).reshape(4, 4, 2, 16, 512)
            return carry

        lax.fori_loop(0, 2, one, 0)

    for k in range(3):
        sent = []
        views = []
        for s in range(3):
            order = GATHER_ORDER[s][::-1]
            e = order[k]
            whole, one, two = col_parts(s)
            width, half = COLS[s][1], SPLIT[s]

            def group(delta, cut, e=e, order=order, k=k):
                at = {d: (me[d] if d in order[:k] else None) for d in order}
                at[e] = coord(e, delta)
                return part.at[rank_index(at) + cut]

            left, left_one = lefts[3 * s + k], left_ones[3 * s + k]
            right, right_one = rights[3 * s + k], right_ones[3 * s + k]
            lead = (slice(None),) * (len(left.shape) - 1)
            left_a = left.at[lead + (pl.ds(0, half),)]
            left_b = left.at[lead + (pl.ds(half, width - half),)]
            right_a = right.at[lead + (pl.ds(0, half),)]
            right_b = right.at[lead + (pl.ds(half, width - half),)]
            sent.append(
                [
                    send(group(2, one), left_one, e, 1),
                    send(group(2, two), right_one, e, -1),
                    send(group(1, two), left_b, e, 1),
                    send(group(-1, one), right_a, e, -1),
                ]
            )
            views.append((group, e, one, two, whole, left_one, right_one, left_a, right_b, left, right))
        for s in range(3):
            group, e, one, two, whole, left_one, right_one, left_a, right_b, left, right = views[s]
            sent[s][0].wait_recv()
            v = group(1, one)
            v[...] = (v[...].astype(F32) + left_one[...].astype(F32)).astype(BF)
            sent[s].append(send(v, left_a, e, 1))
            sent[s][1].wait_recv()
            v = group(-1, two)
            v[...] = (v[...].astype(F32) + right_one[...].astype(F32)).astype(BF)
            sent[s].append(send(v, right_b, e, -1))
        for s in range(3):
            group, e, one, two, whole, left_one, right_one, left_a, right_b, left, right = views[s]
            for copy in sent[s][2:]:
                copy.wait_recv()
            v = group(0, whole)
            total = (
                v[...].astype(F32) + left[...].astype(F32) + right[...].astype(F32)
            )
            if k < 2:
                v[...] = total.astype(BF)
            else:
                low[whole] = total

    for copy in mom_in:
        copy.wait()
    m, h = lax.div(x, 2), lax.rem(x, 2)
    rows = pl.ds(pl.multiple_of(h * 16, 16), 16)
    got = low[...]
    lowx[m, h] = got.astype(BF)
    new_first = beta_first * moms[m, rows] + (1.0 - beta_first) * got
    new_second = beta_second * moms[2 + m, rows] + (1.0 - beta_second) * got * got
    direc[rank_index(me)] = (new_first / jnp.sqrt(new_second)).astype(BF)

    direcs = gather(direc, rank_index, col_parts)
    next(direcs)
    low_view = lowx.at[m, h]
    low_sent = (send(low_view, low_view, "x", 1), send(low_view, low_view, "x", -1))
    next(direcs)
    next(direcs)
    low_sent[0].wait_recv()
    xl = coord("x", -1)
    view = lowx.at[lax.div(xl, 2), lax.rem(xl, 2), :, pl.ds(0, 512)]
    low_a = send(view, view, "x", 1)
    low_sent[1].wait_recv()
    xr = coord("x", 1)
    view = lowx.at[lax.div(xr, 2), lax.rem(xr, 2), :, pl.ds(512, 512)]
    low_b = send(view, view, "x", -1)
    next(direcs)
    next(direcs)
    next(direcs)
    next(masts)
    next(direcs)

    for m in range(2):

        def add(z, acc):
            v = direc[m, z].astype(F32)
            v = jnp.sum((v * v).reshape(16, 8, 1024), axis=0)
            for j in range(8):
                acc = acc + v[:, 128 * j : 128 * (j + 1)]
            return acc

        sq_own[m] = lax.fori_loop(0, 4, add, jnp.zeros((8, 128), F32))
    swapped = send(sq_own, sq_other, "core", 0)
    low_a.wait_recv()
    low_b.wait_recv()
    next(masts)
    swapped.wait_recv()
    sq[...] = sq_own[...] + sq_other[...]
    for copy in started:
        copy.wait_send()


def update_kernel(
    fac,
    direc,
    mast,
    lowx,
    sq,
    first_rec,
    first_gate,
    second_rec,
    second_gate,
    upd_rec,
    upd_gate,
    nf_rec,
    nf_gate,
    ns_rec,
    ns_gate,
    copy_rec,
    copy_gate,
):
    i = pl.program_id(0)
    f = lax.axis_index("fs")

    def scale_of(m):
        total = jnp.sum(sq[m], keepdims=True)
        return 1.0 / jnp.sqrt(total / ENTRIES + scale_floor)

    scales = [scale_of(m) for m in range(2)]

    @pl.when(i == 0)
    def _():
        own = pl.ds(pl.multiple_of(f * 128, 128), 128)
        for m, (upd, nf, ns, first, second) in enumerate(
            (
                (upd_rec, nf_rec, ns_rec, first_rec, second_rec),
                (upd_gate, nf_gate, ns_gate, first_gate, second_gate),
            )
        ):
            got = jnp.dot(
                fac[own, 512 * m : 512 * (m + 1)],
                direc[m],
                preferred_element_type=F32,
            )
            upd[...] = got * scales[m]
            low = lowx[m].astype(F32)
            nf[...] = beta_first * first[...] + (1.0 - beta_first) * low
            ns[...] = beta_second * second[...] + (1.0 - beta_second) * low * low

    rows = pl.ds(pl.multiple_of(i * 256, 256), 256)
    for m, out in enumerate((copy_rec, copy_gate)):
        got = jnp.dot(
            fac[rows, 512 * m : 512 * (m + 1)], direc[m], preferred_element_type=F32
        )
        upd = got * scales[m]
        old = mast[rows, 1024 * m : 1024 * (m + 1)].astype(F32)
        out[...] = (old - step_rate * upd).astype(BF)


def recv_shapes(extra):
    dims = {"x": (2, 2), "y": 4, "z": 4}
    out = []
    for s in range(3):
        order = GATHER_ORDER[s][::-1]
        for k in range(3):
            free = order[k + 1 :]
            lead = []
            if "x" in free:
                lead.append(2)
            if "z" in free:
                lead.append(4)
            if "y" in free:
                lead.append(4)
            if "x" in free:
                lead.append(2)
            width = {
                "all": COLS[s][1],
                "one": SPLIT[s],
                "two": COLS[s][1] - SPLIT[s],
            }[extra]
            out.append(pltpu.VMEM((*lead, 16, width), BF))
    return out


def body(
    normed_in,
    cotan_rec,
    cotan_gate,
    factor_rec,
    factor_gate,
    first_rec,
    first_gate,
    second_rec,
    second_gate,
    master_rec,
    master_gate,
):
    hbm = pl.BlockSpec(memory_space=pl.ANY)
    vmem = pl.BlockSpec(memory_space=pltpu.VMEM)
    fac, direc, mast, lowx, sq = pl.pallas_call(
        ring_kernel,
        name="rings",
        out_shape=(
            jax.ShapeDtypeStruct((4, 4, 4, 2, 16, 1024), BF),
            jax.ShapeDtypeStruct((2, 4, 4, 2, 16, 1024), BF),
            jax.ShapeDtypeStruct((4, 4, 4, 32, 2048), BF),
            jax.ShapeDtypeStruct((2, 2, 16, 1024), BF),
            jax.ShapeDtypeStruct((2, 8, 128), F32),
        ),
        in_specs=[hbm] * 11,
        out_specs=(vmem,) * 5,
        scratch_shapes=[
            pltpu.VMEM((6, 256, D), BF),
            pltpu.VMEM((2, TOK, HALF), BF),
            pltpu.VMEM((2, RANK, TOK), BF),
            pltpu.VMEM((2, 4, 4, 2, 16, 1024), BF),
            pltpu.VMEM((4, 32, 1024), F32),
            pltpu.VMEM((2, 32, 1024), F32),
            pltpu.VMEM((16, 1024), F32),
            pltpu.VMEM((2, 8, 128), F32),
            pltpu.VMEM((2, 8, 128), F32),
            recv_shapes("all"),
            recv_shapes("one"),
            recv_shapes("all"),
            recv_shapes("two"),
            pltpu.SemaphoreType.DMA((N_SEMS,)),
            pltpu.SemaphoreType.DMA((N_SEMS,)),
            pltpu.SemaphoreType.DMA((16,)),
        ],
        compiler_params=pltpu.CompilerParams(
            collective_id=0, has_side_effects=True, vmem_limit_bytes=52 << 20
        ),
    )(
        normed_in,
        cotan_rec,
        cotan_gate,
        factor_rec,
        factor_gate,
        first_rec,
        first_gate,
        second_rec,
        second_gate,
        master_rec,
        master_gate,
    )
    fac = fac.reshape(D, 2 * RANK)
    direc = direc.reshape(2, RANK, HALF)
    mast = mast.reshape(D, 2 * HALF)
    lowx = lowx.reshape(2, 32, HALF)

    def once(shape):
        return pl.BlockSpec(shape, lambda i: (0,) * len(shape))

    row = pl.BlockSpec((256, HALF), lambda i: (i, 0))
    return pl.pallas_call(
        update_kernel,
        name="update",
        grid=(8,),
        out_shape=(
            *(jax.ShapeDtypeStruct((128, HALF), F32),) * 2,
            *(jax.ShapeDtypeStruct((32, HALF), F32),) * 4,
            *(jax.ShapeDtypeStruct((D, HALF), BF),) * 2,
        ),
        in_specs=[vmem] * 9,
        out_specs=(*(once((128, HALF)),) * 2, *(once((32, HALF)),) * 4, row, row),
        compiler_params=pltpu.CompilerParams(vmem_limit_bytes=48 << 20),
    )(fac, direc, mast, lowx, sq, first_rec, first_gate, second_rec, second_gate)


def solution(mesh):
    return jax.shard_map(
        body,
        mesh=mesh,
        in_specs=(
            P(("fs", "rep"), None),
            P(("fs", "rep"), "tp"),
            P(("fs", "rep"), "tp"),
            P("fs", None),
            P("fs", None),
            P("fs", "tp"),
            P("fs", "tp"),
            P("fs", "tp"),
            P("fs", "tp"),
            P("fs", "tp"),
            P("fs", "tp"),
        ),
        out_specs=(
            P("fs", "tp"),
            P("fs", "tp"),
            P("fs", "tp"),
            P("fs", "tp"),
            P("fs", "tp"),
            P("fs", "tp"),
            P(None, "tp"),
            P(None, "tp"),
        ),
        check_vma=False,
    )
```

```python
import jax
import jax.numpy as jnp
from jax import lax
from jax.experimental import pallas as pl
from jax.experimental.pallas import tpu as pltpu
from jax.sharding import PartitionSpec as P

MESH = pl.DeviceIdType.MESH
BF = jnp.bfloat16
F32 = jnp.float32

D = 2048
DR = 2048
RANK = 512
ENTRIES = float(RANK * DR)
TOK = 1536
HALF = 1024

beta_first = 0.8
beta_second = 0.9
scale_floor = 0.25
step_rate = 0.01

GATHER_ORDER = (("x", "y", "z"), ("y", "z", "x"), ("z", "x", "y"))
COLS = ((0, 384), (384, 384), (768, 256))
SPLIT = (256, 128, 128)
WIDE_COLS = ((0, 640), (640, 640), (1280, 768))
N_SEMS = 172


def ring_kernel(
    normed_ref,
    cot_rec_ref,
    cot_gate_ref,
    fac_rec_ref,
    fac_gate_ref,
    first_rec_ref,
    first_gate_ref,
    second_rec_ref,
    second_gate_ref,
    master_rec_ref,
    master_gate_ref,
    fac,
    direc,
    mast,
    lowx,
    sq,
    xs,
    cots,
    proj_t,
    part,
    moms,
    mast_f,
    low,
    sq_own,
    sq_other,
    lefts,
    left_ones,
    rights,
    right_ones,
    send_sems,
    recv_sems,
    local_sems,
):
    f, x, c = lax.axis_index("fs"), lax.axis_index("rep"), lax.axis_index("tp")
    me = {"x": x, "y": lax.rem(f, 4), "z": lax.div(f, 4)}
    count = [0]
    started = []

    def coord(dim, delta):
        return lax.rem(me[dim] + (delta + 4) % 4, 4)

    def device(dim, delta):
        if dim == "core":
            return {"tp": 1 - c}
        p = coord(dim, delta)
        if dim == "x":
            return {"rep": p}
        if dim == "y":
            return {"fs": me["z"] * 4 + p}
        return {"fs": p * 4 + me["y"]}

    def send(src, dst, dim, delta):
        k = count[0]
        count[0] += 1
        copy = pltpu.make_async_remote_copy(
            src_ref=src,
            dst_ref=dst,
            send_sem=send_sems.at[k],
            recv_sem=recv_sems.at[k],
            device_id=device(dim, delta),
            device_id_type=MESH,
        )
        copy.start()
        started.append(copy)
        return copy

    def full(v):
        return slice(None) if v is None else v

    def rank_index(at):
        xx = at["x"]
        if xx is None:
            return (slice(None), full(at["z"]), full(at["y"]), slice(None))
        return (lax.div(xx, 2), full(at["z"]), full(at["y"]), lax.rem(xx, 2))

    def fac_index(at):
        return (full(at["z"]), full(at["y"]), full(at["x"]), c)

    def mast_index(at):
        return (full(at["z"]), full(at["y"]), full(at["x"]))

    def col_parts(s):
        base, width = COLS[s]
        one = SPLIT[s]
        rows = slice(None)
        return (
            (rows, pl.ds(base, width)),
            (rows, pl.ds(base, one)),
            (rows, pl.ds(base + one, width - one)),
        )

    def row_parts(s):
        base, width = WIDE_COLS[s]
        cols = pl.ds(base, width)
        return ((slice(None), cols), (pl.ds(0, 16), cols), (pl.ds(16, 16), cols))

    def gather(buf, index, parts):
        for k in range(3):
            sent = []
            for s in range(3):
                order = GATHER_ORDER[s]
                at = {d: (None if d in order[:k] else me[d]) for d in order}
                whole, _, _ = parts(s)
                view = buf.at[index(at) + whole]
                sent.append(
                    (send(view, view, order[k], 1), send(view, view, order[k], -1))
                )
            yield
            passed = []
            for s in range(3):
                order = GATHER_ORDER[s]
                _, one, two = parts(s)
                at = {d: (None if d in order[:k] else me[d]) for d in order}
                sent[s][0].wait_recv()
                at[order[k]] = coord(order[k], -1)
                view = buf.at[index(at) + one]
                a = send(view, view, order[k], 1)
                sent[s][1].wait_recv()
                at[order[k]] = coord(order[k], 1)
                view = buf.at[index(at) + two]
                b = send(view, view, order[k], -1)
                passed.append((a, b))
            yield
            for a, b in passed:
                a.wait_recv()
                b.wait_recv()
        yield

    local = []

    def fetch(src, dst):
        copy = pltpu.make_async_copy(src, dst, local_sems.at[len(local)])
        copy.start()
        local.append(copy)
        return copy

    own_rows = pl.ds(pl.multiple_of((2 * x + c) * 16, 16), 16)
    own_fac = fac_index(me)
    fac_in = [
        fetch(r.at[own_rows], fac.at[own_fac + (slice(None), pl.ds(512 * m, 512))])
        for m, r in enumerate((fac_rec_ref, fac_gate_ref))
    ]
    quarter = pl.ds(pl.multiple_of(x * 32, 32), 32)
    mast_in = [
        fetch(r.at[quarter], mast_f.at[m])
        for m, r in enumerate((master_rec_ref, master_gate_ref))
    ]
    x_in = [
        fetch(normed_ref.at[pl.ds(256 * i, 256)], xs.at[i]) for i in range(6)
    ]
    cot_in = [fetch(r, cots.at[m]) for m, r in enumerate((cot_rec_ref, cot_gate_ref))]
    mom_in = [
        fetch(r, moms.at[i])
        for i, r in enumerate(
            (first_rec_ref, first_gate_ref, second_rec_ref, second_gate_ref)
        )
    ]

    barrier = pltpu.get_barrier_semaphore()
    for dim, delta in (("x", 1), ("x", -1), ("y", 1), ("y", -1), ("z", 1), ("z", -1), ("core", 0)):
        pl.semaphore_signal(
            barrier, inc=1, device_id=device(dim, delta), device_id_type=MESH
        )
    for copy in mast_in:
        copy.wait()
    own_mast = mast_index(me)
    for m in range(2):
        mast[own_mast + (slice(None), pl.ds(1024 * m, 1024))] = mast_f[m].astype(BF)
    for copy in fac_in:
        copy.wait()
    with jax.named_scope("barrier"):
        pl.semaphore_wait(barrier, 7)

    facs = gather(fac, fac_index, col_parts)
    masts = gather(mast, mast_index, row_parts)

    def step(it, name):
        with jax.named_scope(name):
            next(it)

    for i in range(2):
        step(facs, f"fac{i}")
        step(masts, f"mast{i}")
    for i in range(2, 6):
        step(facs, f"fac{i}")
    step(masts, "mast2")
    step(facs, "fac6")
    swap = []
    for s in range(3):
        whole = col_parts(s)[0]
        view = fac.at[(slice(None), slice(None), slice(None), c) + whole]
        swap.append(send(view, view, "core", 0))
    step(masts, "mast3")
    with jax.named_scope("swap"):
        for copy in swap:
            copy.wait_recv()
    with jax.named_scope("xin"):
        for copy in x_in:
            copy.wait()

    def project(lo, hi):
        def one(i, carry):
            tokens = pl.ds(pl.multiple_of(i * 256, 256), 256)
            for m in range(2):
                cols = pl.ds(512 * m, 512)
                factor = fac[:, :, :, :, :, cols].reshape(D, 512)
                got = jnp.dot(xs[i], factor, preferred_element_type=F32)
                proj_t[m, :, tokens] = got.astype(BF).T
            return carry

        lax.fori_loop(lo, hi, one, 0)

    with jax.named_scope("proj0"):
        project(0, 3)
    step(masts, "mast4")
    with jax.named_scope("proj1"):
        project(3, 6)
    for copy in cot_in:
        copy.wait()

    for m in range(2):

        def one(j, carry):
            cols = pl.ds(pl.multiple_of(j * 512, 512), 512)
            got = jnp.dot(proj_t[m], cots[m, :, cols], preferred_element_type=F32)
            part[m, :, :, :, :, cols] = got.astype(BF).reshape(4, 4, 2, 16, 512)
            return carry

        with jax.named_scope("part"):
            lax.fori_loop(0, 2, one, 0)

    for k in range(3):
        sent = []
        views = []
        for s in range(3):
            order = GATHER_ORDER[s][::-1]
            e = order[k]
            whole, one, two = col_parts(s)
            width, half = COLS[s][1], SPLIT[s]

            def group(delta, cut, e=e, order=order, k=k):
                at = {d: (me[d] if d in order[:k] else None) for d in order}
                at[e] = coord(e, delta)
                return part.at[rank_index(at) + cut]

            left, left_one = lefts[3 * s + k], left_ones[3 * s + k]
            right, right_one = rights[3 * s + k], right_ones[3 * s + k]
            lead = (slice(None),) * (len(left.shape) - 1)
            left_a = left.at[lead + (pl.ds(0, half),)]
            left_b = left.at[lead + (pl.ds(half, width - half),)]
            right_a = right.at[lead + (pl.ds(0, half),)]
            right_b = right.at[lead + (pl.ds(half, width - half),)]
            sent.append(
                [
                    send(group(2, one), left_one, e, 1),
                    send(group(2, two), right_one, e, -1),
                    send(group(1, two), left_b, e, 1),
                    send(group(-1, one), right_a, e, -1),
                ]
            )
            views.append((group, e, one, two, whole, left_one, right_one, left_a, right_b, left, right))
        mark = jax.named_scope(f"rs_pass{k}")
        mark.__enter__()
        for s in range(3):
            group, e, one, two, whole, left_one, right_one, left_a, right_b, left, right = views[s]
            sent[s][0].wait_recv()
            v = group(1, one)
            v[...] = (v[...].astype(F32) + left_one[...].astype(F32)).astype(BF)
            sent[s].append(send(v, left_a, e, 1))
            sent[s][1].wait_recv()
            v = group(-1, two)
            v[...] = (v[...].astype(F32) + right_one[...].astype(F32)).astype(BF)
            sent[s].append(send(v, right_b, e, -1))
        mark.__exit__(None, None, None)
        mark = jax.named_scope(f"rs_sum{k}")
        mark.__enter__()
        for s in range(3):
            group, e, one, two, whole, left_one, right_one, left_a, right_b, left, right = views[s]
            for copy in sent[s][2:]:
                copy.wait_recv()
            v = group(0, whole)
            total = (
                v[...].astype(F32) + left[...].astype(F32) + right[...].astype(F32)
            )
            if k < 2:
                v[...] = total.astype(BF)
            else:
                low[whole] = total
        mark.__exit__(None, None, None)

    for copy in mom_in:
        copy.wait()
    m, h = lax.div(x, 2), lax.rem(x, 2)
    rows = pl.ds(pl.multiple_of(h * 16, 16), 16)
    got = low[...]
    lowx[m, h] = got.astype(BF)
    new_first = beta_first * moms[m, rows] + (1.0 - beta_first) * got
    new_second = beta_second * moms[2 + m, rows] + (1.0 - beta_second) * got * got
    direc[rank_index(me)] = (new_first / jnp.sqrt(new_second)).astype(BF)

    direcs = gather(direc, rank_index, col_parts)
    step(direcs, "dir0")
    low_view = lowx.at[m, h]
    low_sent = (send(low_view, low_view, "x", 1), send(low_view, low_view, "x", -1))
    step(direcs, "dir1")
    step(direcs, "dir2")
    low_sent[0].wait_recv()
    xl = coord("x", -1)
    view = lowx.at[lax.div(xl, 2), lax.rem(xl, 2), :, pl.ds(0, 512)]
    low_a = send(view, view, "x", 1)
    low_sent[1].wait_recv()
    xr = coord("x", 1)
    view = lowx.at[lax.div(xr, 2), lax.rem(xr, 2), :, pl.ds(512, 512)]
    low_b = send(view, view, "x", -1)
    step(direcs, "dir3")
    step(direcs, "dir4")
    step(direcs, "dir5")
    step(masts, "mast5")
    step(direcs, "dir6")

    for m in range(2):

        def add(z, acc):
            v = direc[m, z].astype(F32)
            v = jnp.sum((v * v).reshape(16, 8, 1024), axis=0)
            for j in range(8):
                acc = acc + v[:, 128 * j : 128 * (j + 1)]
            return acc

        with jax.named_scope("squares"):
            sq_own[m] = lax.fori_loop(0, 4, add, jnp.zeros((8, 128), F32))
    swapped = send(sq_own, sq_other, "core", 0)
    low_a.wait_recv()
    low_b.wait_recv()
    step(masts, "mast6")
    swapped.wait_recv()
    sq[...] = sq_own[...] + sq_other[...]
    with jax.named_scope("drain"):
        for copy in started:
            copy.wait_send()


def update_kernel(
    fac,
    direc,
    mast,
    lowx,
    sq,
    first_rec,
    first_gate,
    second_rec,
    second_gate,
    upd_rec,
    upd_gate,
    nf_rec,
    nf_gate,
    ns_rec,
    ns_gate,
    copy_rec,
    copy_gate,
):
    i = pl.program_id(0)
    f = lax.axis_index("fs")

    def scale_of(m):
        total = jnp.sum(sq[m], keepdims=True)
        return 1.0 / jnp.sqrt(total / ENTRIES + scale_floor)

    scales = [scale_of(m) for m in range(2)]

    @pl.when(i == 0)
    def _():
        own = pl.ds(pl.multiple_of(f * 128, 128), 128)
        for m, (upd, nf, ns, first, second) in enumerate(
            (
                (upd_rec, nf_rec, ns_rec, first_rec, second_rec),
                (upd_gate, nf_gate, ns_gate, first_gate, second_gate),
            )
        ):
            got = jnp.dot(
                fac[own, 512 * m : 512 * (m + 1)],
                direc[m],
                preferred_element_type=F32,
            )
            upd[...] = got * scales[m]
            low = lowx[m].astype(F32)
            nf[...] = beta_first * first[...] + (1.0 - beta_first) * low
            ns[...] = beta_second * second[...] + (1.0 - beta_second) * low * low

    rows = pl.ds(pl.multiple_of(i * 256, 256), 256)
    for m, out in enumerate((copy_rec, copy_gate)):
        got = jnp.dot(
            fac[rows, 512 * m : 512 * (m + 1)], direc[m], preferred_element_type=F32
        )
        upd = got * scales[m]
        old = mast[rows, 1024 * m : 1024 * (m + 1)].astype(F32)
        out[...] = (old - step_rate * upd).astype(BF)


def recv_shapes(extra):
    dims = {"x": (2, 2), "y": 4, "z": 4}
    out = []
    for s in range(3):
        order = GATHER_ORDER[s][::-1]
        for k in range(3):
            free = order[k + 1 :]
            lead = []
            if "x" in free:
                lead.append(2)
            if "z" in free:
                lead.append(4)
            if "y" in free:
                lead.append(4)
            if "x" in free:
                lead.append(2)
            width = {
                "all": COLS[s][1],
                "one": SPLIT[s],
                "two": COLS[s][1] - SPLIT[s],
            }[extra]
            out.append(pltpu.VMEM((*lead, 16, width), BF))
    return out


def body(
    normed_in,
    cotan_rec,
    cotan_gate,
    factor_rec,
    factor_gate,
    first_rec,
    first_gate,
    second_rec,
    second_gate,
    master_rec,
    master_gate,
):
    hbm = pl.BlockSpec(memory_space=pltpu.HBM)
    vmem = pl.BlockSpec(memory_space=pltpu.VMEM)
    fac, direc, mast, lowx, sq = pl.pallas_call(
        ring_kernel,
        name="rings",
        out_shape=(
            pltpu.VMEM((4, 4, 4, 2, 16, 1024), BF),
            pltpu.VMEM((2, 4, 4, 2, 16, 1024), BF),
            pltpu.VMEM((4, 4, 4, 32, 2048), BF),
            pltpu.VMEM((2, 2, 16, 1024), BF),
            pltpu.VMEM((2, 8, 128), F32),
        ),
        in_specs=[hbm] * 11,
        out_specs=(vmem,) * 5,
        scratch_shapes=[
            pltpu.VMEM((6, 256, D), BF),
            pltpu.VMEM((2, TOK, HALF), BF),
            pltpu.VMEM((2, RANK, TOK), BF),
            pltpu.VMEM((2, 4, 4, 2, 16, 1024), BF),
            pltpu.VMEM((4, 32, 1024), F32),
            pltpu.VMEM((2, 32, 1024), F32),
            pltpu.VMEM((16, 1024), F32),
            pltpu.VMEM((2, 8, 128), F32),
            pltpu.VMEM((2, 8, 128), F32),
            recv_shapes("all"),
            recv_shapes("one"),
            recv_shapes("all"),
            recv_shapes("two"),
            pltpu.SemaphoreType.DMA((N_SEMS,)),
            pltpu.SemaphoreType.DMA((N_SEMS,)),
            pltpu.SemaphoreType.DMA((16,)),
        ],
        compiler_params=pltpu.CompilerParams(
            collective_id=0, has_side_effects=True, vmem_limit_bytes=40 << 20
        ),
    )(
        normed_in,
        cotan_rec,
        cotan_gate,
        factor_rec,
        factor_gate,
        first_rec,
        first_gate,
        second_rec,
        second_gate,
        master_rec,
        master_gate,
    )
    fac = fac.reshape(D, 2 * RANK)
    direc = direc.reshape(2, RANK, HALF)
    mast = mast.reshape(D, 2 * HALF)
    lowx = lowx.reshape(2, 32, HALF)

    def once(shape):
        return pl.BlockSpec(shape, lambda i: (0,) * len(shape))

    row = pl.BlockSpec((256, HALF), lambda i: (i, 0))
    return pl.pallas_call(
        update_kernel,
        name="update",
        grid=(8,),
        out_shape=(
            *(jax.ShapeDtypeStruct((128, HALF), F32),) * 2,
            *(jax.ShapeDtypeStruct((32, HALF), F32),) * 4,
            *(jax.ShapeDtypeStruct((D, HALF), BF),) * 2,
        ),
        in_specs=[vmem] * 9,
        out_specs=(*(once((128, HALF)),) * 2, *(once((32, HALF)),) * 4, row, row),
        compiler_params=pltpu.CompilerParams(vmem_limit_bytes=24 << 20),
    )(fac, direc, mast, lowx, sq, first_rec, first_gate, second_rec, second_gate)


def solution(mesh):
    return jax.shard_map(
        body,
        mesh=mesh,
        in_specs=(
            P(("fs", "rep"), None),
            P(("fs", "rep"), "tp"),
            P(("fs", "rep"), "tp"),
            P("fs", None),
            P("fs", None),
            P("fs", "tp"),
            P("fs", "tp"),
            P("fs", "tp"),
            P("fs", "tp"),
            P("fs", "tp"),
            P("fs", "tp"),
        ),
        out_specs=(
            P("fs", "tp"),
            P("fs", "tp"),
            P("fs", "tp"),
            P("fs", "tp"),
            P("fs", "tp"),
            P("fs", "tp"),
            P(None, "tp"),
            P(None, "tp"),
        ),
        check_vma=False,
    )
```
